32 devices in a mesh: fs: 8 (over z, y), tp: 4 (over x, core).
Axes of the slice: x: 2, y: 2, z: 4, core: 2. Of those that a mesh axis runs over, the one named last changes fastest.
Arguments:
- mixed: bfloat16 [12288, 2048], P(('fs', 'tp')), may hold values from -6 to 6
- residual: bfloat16 [12288, 2048], P(('fs', 'tp')), may hold values from -6 to 6
- mix_weight: bfloat16 [2048, 2048], P(('fs', 'tp')), may hold values from -0.125 to 0.125
- norm_gain: float32 [2048], replicated, may hold values from 0.1 to 1.9
- up_weight: bfloat16 [2048, 5504], P('fs', 'tp'), may hold values from -0.125 to 0.125
- gate_weight: bfloat16 [2048, 5504], P('fs', 'tp'), may hold values from -0.125 to 0.125
- conv_weight: float32 [3, 5504], P(None, 'tp'), may hold values from -3 to 3
- conv_bias: float32 [5504], P('tp'), may hold values from -3 to 3
- down_weight: bfloat16 [5504, 2048], P('tp', 'fs'), may hold values from -0.078125 to 0.078125
Outputs:
- output: bfloat16 [12288, 2048], P(('fs', 'tp'))
The draws below stay inside these ranges and needn't reach their ends.
All inputs are finite; a program needn't handle non-finite values.
Results may differ from the reference program's by a relative error of at most 0.012.
Values may be sent and summed in bfloat16 or wider, within the bound.
A program may use at most 128 MiB of HBM per device.

```python
import jax
import jax.numpy as jnp
from jax import lax

D = 2048
DM = 2048
FF = 5504
TOK_DEV = 384
TOKENS = 12288
N_FS = 8
N_TP = 4


def block_levels(stream_key, dims, shards, smallest, top_value):
    factor_of = 1.0
    for axis_at, parts in shards:
        steps = jax.random.uniform(jax.random.fold_in(jax.random.fold_in(stream_key, 6), axis_at), (parts,), jnp.float32, smallest / len(shards), top_value / len(shards))
        factor_of = factor_of * jnp.repeat(jnp.exp(steps), dims[axis_at] // parts).reshape((-1,) + (1,) * (len(dims) - 1 - axis_at))
    return factor_of


def scatter_about(own_key, shape, width, bound, pieces=(), kind=jnp.bfloat16):
    loudness = block_levels(own_key, shape, pieces, -0.22, 0.18) if pieces else 1.0
    entries = jax.random.normal(own_key, shape, jnp.float32) * width * loudness
    return jnp.minimum(jnp.maximum(entries, -bound), bound).astype(kind)


def setup_inputs(seed: int = 0) -> dict:
    streams_of = jax.random.split(jax.random.key(seed), 10)
    return {
        "mixed": scatter_about(streams_of[0], (TOKENS, DM), 1.0, 6.0, ((0, 32),)),
        "residual": scatter_about(streams_of[1], (TOKENS, D), 1.0, 6.0, ((0, 32),)),
        "mix_weight": scatter_about(streams_of[2], (DM, D), DM ** -0.5, 0.125, ((0, 32),)),
        "norm_gain": jnp.clip(1.0 + 0.18 * jax.random.normal(streams_of[3], (D,), jnp.float32), 0.1, 1.9),
        "up_weight": scatter_about(streams_of[4], (D, FF), D ** -0.5, 0.125, ((0, 8), (1, 4))),
        "gate_weight": scatter_about(streams_of[5], (D, FF), D ** -0.5, 0.125, ((0, 8), (1, 4))),
        "conv_weight": scatter_about(streams_of[6], (3, FF), 0.577, 3.0, ((1, 4),), jnp.float32),
        "conv_bias": scatter_about(streams_of[7], (FF,), 0.5, 3.0, ((0, 4),), jnp.float32),
        "down_weight": scatter_about(streams_of[8], (FF, D), FF ** -0.5, 0.078125, ((0, 4), (1, 8))),
    }


norm_eps = 1e-06

def reference(mixed, residual, mix_weight, norm_gain, up_weight, gate_weight, conv_weight, conv_bias, down_weight):
    unit_block = FF // N_TP
    length = TOK_DEV * N_TP
    stream = (residual.astype(jnp.float32) + jnp.dot(mixed, mix_weight, preferred_element_type=jnp.float32)).astype(jnp.bfloat16)
    x_float = stream.astype(jnp.float32)
    normed = (x_float * lax.rsqrt(lax.optimization_barrier(jnp.mean(x_float * x_float, axis=-1, keepdims=True)) + norm_eps) * norm_gain).astype(jnp.bfloat16)

    def one_seq(pair):
        normed_seq, stream_seq = pair
        up_part = jnp.dot(normed_seq, up_weight, preferred_element_type=jnp.float32).astype(jnp.bfloat16)
        gate_part = jnp.dot(normed_seq, gate_weight, preferred_element_type=jnp.float32).astype(jnp.bfloat16)
        up_float = lax.optimization_barrier(up_part).astype(jnp.float32)
        padded = jnp.pad(up_float, ((2, 0), (0, 0)))
        smoothed = conv_bias + conv_weight[0] * padded[:-2] + conv_weight[1] * padded[1:-1] + conv_weight[2] * padded[2:]
        hidden = (jax.nn.gelu(smoothed) * gate_part.astype(jnp.float32)).astype(jnp.bfloat16)
        accum_sum = stream_seq.astype(jnp.float32)
        for index in range(N_TP):
            partial_value = jnp.dot(hidden[:, index * unit_block:(index + 1) * unit_block], down_weight[index * unit_block:(index + 1) * unit_block], preferred_element_type=jnp.float32).astype(jnp.bfloat16)
            accum_sum = accum_sum + lax.optimization_barrier(partial_value).astype(jnp.float32)
        return accum_sum.astype(jnp.bfloat16)
    result = lax.map(one_seq, (normed.reshape(N_FS, length, D), stream.reshape(N_FS, length, D)))
    return result.reshape(N_FS * length, D)
```

```python
import jax
import jax.numpy as jnp
from jax import lax
from jax.sharding import PartitionSpec as P

norm_eps = 1e-06
f32, bf16 = jnp.float32, jnp.bfloat16


def make_body(n_fs, n_tp, ny):
    nz, nx = n_fs // ny, n_tp // 2
    line = nz == 4
    if line:
        zord = [[0, 1, 2, 3], [1, 0, 2, 3], [2, 3, 1, 0], [3, 2, 1, 0]]
    else:
        zord = [[(z + d) % nz for d in range(nz)] for z in range(nz)]
    order = [
        [zord[z][s] * ny + (y + dy) % ny for s in range(nz) for dy in range(ny)]
        for z in range(nz)
        for y in range(ny)
    ]

    def hop_z(a, pairs):
        return lax.ppermute(a, "fs", [(s * ny + y, t * ny + y) for s, t in pairs for y in range(ny)])

    def hop_y(a, dy):
        return lax.ppermute(
            a, "fs", [(z * ny + (y + dy) % ny, z * ny + y) for z in range(nz) for y in range(ny)]
        )

    def hop_x(a, dx):
        return lax.ppermute(
            a, "tp", [(x * 2 + c, (x + dx) % nx * 2 + c) for x in range(nx) for c in range(2)]
        )

    def hop_core(a):
        return lax.ppermute(a, "tp", [(t, t ^ 1) for t in range(n_tp)])

    def z_gather(own):
        if not line:
            return [own] + [hop_z(own, [((z + d) % nz, z) for z in range(nz)]) for d in range(1, nz)]
        z = lax.axis_index("fs") // ny
        mid = (z == 1) | (z == 2)
        s1 = hop_z(own, [(0, 1), (1, 0), (2, 3), (3, 2)])
        s2m = hop_z(own, [(1, 2), (2, 1)])
        s3m = hop_z(s1, [(1, 2), (2, 1)])
        s2e = hop_z(s2m, [(1, 0), (2, 3)])
        s3e = hop_z(s3m, [(1, 0), (2, 3)])
        return [own, s1, jnp.where(mid, s2m, s2e), jnp.where(mid, s3m, s3e)]

    def fs_gather(own, y_first=False):
        if y_first:
            cols = [z_gather(own)] + [z_gather(hop_y(own, dy)) for dy in range(1, ny)]
            return [cols[dy][s] for s in range(nz) for dy in range(ny)]
        pieces = []
        for p in z_gather(own):
            pieces += [p] + [hop_y(p, dy) for dy in range(1, ny)]
        return pieces

    def body(
        mixed,
        residual,
        mix_weight,
        norm_gain,
        up_weight,
        gate_weight,
        conv_weight,
        conv_bias,
        down_weight,
    ):
        fs_i, tp_i = lax.axis_index("fs"), lax.axis_index("tp")
        core, x_i = tp_i % 2, tp_i // 2
        slots = jnp.array(order, jnp.int32)[fs_i]
        tok, width = residual.shape
        mrow = mix_weight.shape[0]
        own = jnp.concatenate(fs_gather(mix_weight), axis=0)
        parts = [own] + [hop_x(own, dx) for dx in range(1, nx)]
        parts = parts + [hop_core(p) for p in parts]
        owners = [((x_i - dx) % nx) * 2 + core for dx in range(nx)]
        owners = owners + [o ^ 1 for o in owners]
        mt = mixed.reshape(tok, n_fs, n_tp, mrow).transpose(2, 1, 0, 3)
        mt = jnp.concatenate(
            [lax.dynamic_slice_in_dim(mt, slots[j], 1, axis=1) for j in range(n_fs)], axis=1
        )
        mt = lax.optimization_barrier(mt.transpose(0, 2, 1, 3).reshape(n_tp, tok, n_fs * mrow))
        summed = 0.0
        for part, owner in zip(parts, owners):
            summed = summed + jnp.dot(
                lax.dynamic_index_in_dim(mt, owner, 0, keepdims=False), part, preferred_element_type=f32
            )
        stream = (residual.astype(f32) + summed).astype(bf16)
        x_float = stream.astype(f32)
        normed = (
            x_float
            * lax.rsqrt(jnp.mean(x_float * x_float, axis=-1, keepdims=True) + norm_eps)
            * norm_gain
        ).astype(bf16)
        rows = up_weight.shape[0]
        n_c = max(1, rows // 128)
        step = rows // n_c
        normed = jnp.concatenate(
            [
                lax.dynamic_slice_in_dim(normed, slots[j] * rows + c * step, step, axis=1)
                for c in range(n_c)
                for j in range(n_fs)
            ],
            axis=1,
        )

        def gather_rows(w, first):
            out = []
            for c in range(n_c):
                out += fs_gather(w[c * step : (c + 1) * step], y_first=first and c == 0)
            return jnp.concatenate(out, axis=0)

        up_full = gather_rows(up_weight, n_c > 1)
        gate_full = gather_rows(gate_weight, False)
        tokens = lax.all_gather(normed, "tp", axis=0, tiled=True)
        up_part = jnp.dot(tokens, up_full, preferred_element_type=f32).astype(bf16)
        gate_part = jnp.dot(tokens, gate_full, preferred_element_type=f32).astype(bf16)
        up_float = lax.optimization_barrier(up_part).astype(f32)
        padded = jnp.pad(up_float, ((2, 0), (0, 0)))
        smoothed = (
            conv_bias
            + conv_weight[0] * padded[:-2]
            + conv_weight[1] * padded[1:-1]
            + conv_weight[2] * padded[2:]
        )
        hidden = (jax.nn.gelu(smoothed) * gate_part.astype(f32)).astype(bf16)
        hidden = lax.optimization_barrier(hidden)
        cols = down_weight.shape[1]
        d_c = max(1, cols // 128)
        wide = cols // d_c
        sums = []
        for c in range(d_c):
            piece = jnp.concatenate(fs_gather(down_weight[:, c * wide : (c + 1) * wide]), axis=1)
            part = jnp.dot(hidden, piece, preferred_element_type=f32).astype(bf16)
            part = part.reshape(nx, 2, tok, n_fs * wide)
            theirs = lax.dynamic_index_in_dim(part, 1 - core, 1, keepdims=False)
            ours = lax.dynamic_index_in_dim(part, core, 1, keepdims=False)
            pair = (ours.astype(f32) + hop_core(theirs).astype(f32)).astype(bf16)
            total = lax.dynamic_index_in_dim(pair, x_i, 0, keepdims=False).astype(f32)
            for dx in range(1, nx):
                away = lax.dynamic_index_in_dim(pair, (x_i + dx) % nx, 0, keepdims=False)
                total = total + hop_x(away, dx).astype(f32)
            sums.append(total)
        inverse = [[o.index(a) for a in range(n_fs)] for o in order]
        where_at = jnp.array(inverse, jnp.int32)[fs_i]
        summed_out = jnp.concatenate(
            [
                lax.dynamic_slice_in_dim(sums[c], where_at[a] * wide, wide, axis=1)
                for a in range(n_fs)
                for c in range(d_c)
            ],
            axis=1,
        )
        return (x_float + summed_out).astype(bf16)

    return body


def solution(mesh):
    coords = [getattr(d, "coords", None) for d in mesh.devices[:, 0]]
    n_fs, n_tp = mesh.shape["fs"], mesh.shape["tp"]
    ny = len({c[1] for c in coords}) if None not in coords else 1
    if n_fs % ny:
        ny = 1
    return jax.shard_map(
        make_body(n_fs, n_tp, ny),
        mesh=mesh,
        in_specs=(
            P(("fs", "tp"), None),
            P(("fs", "tp"), None),
            P(("fs", "tp"), None),
            P(),
            P("fs", "tp"),
            P("fs", "tp"),
            P(None, "tp"),
            P("tp"),
            P("tp", "fs"),
        ),
        out_specs=P(("fs", "tp"), None),
        check_vma=False,
    )
```

```python
import functools

import jax
import jax.numpy as jnp
from jax import lax
from jax.experimental import pallas as pl
from jax.experimental.pallas import tpu as pltpu
from jax.sharding import PartitionSpec as P

norm_eps = 1e-06
f32, bf16 = jnp.float32, jnp.bfloat16
MESH = pl.DeviceIdType.MESH


def gather_kernel(nz, ny, plan, count, *refs):
    shards, fulls = refs[:count], refs[count : 2 * count]
    send_sem, recv_sem, local_sem = refs[2 * count :]
    n_fs = nz * ny
    me = lax.axis_index("fs")
    z, y = me // ny, lax.rem(me, ny)

    def fs_at(zz, dy):
        return zz * ny + lax.rem(y + dy, ny)

    def piece(c, f):
        m, axis, block, off, size, _ = plan[c]
        if axis == 0:
            return fulls[m].at[pl.ds(pl.multiple_of(f * block + off, 16), size), :]
        return fulls[m].at[:, pl.ds(pl.multiple_of(f * block + off, 128), size)]

    def own(c):
        m, axis, _, off, size, _ = plan[c]
        return shards[m].at[off : off + size, :] if axis == 0 else shards[m].at[:, off : off + size]

    def copy(c, f, lane, to, mine=False):
        return pltpu.make_async_remote_copy(
            src_ref=own(c) if mine else piece(c, f),
            dst_ref=piece(c, f),
            send_sem=send_sem.at[lane, f, c],
            recv_sem=recv_sem.at[f, c],
            device_id={"fs": to},
            device_id_type=MESH,
        )

    def arrived(c, f):
        copy(c, f, 0, lax.rem(me + 1, n_fs)).wait_recv()

    def z_sends(act, c, f, up, down, mine=False):
        if up:

            @pl.when(z < nz - 1)
            def _():
                act(copy(c, f, 0, me + ny, mine))

        if down:

            @pl.when(z > 0)
            def _():
                act(copy(c, f, 1, me - ny, mine))

    def y_sends(act, c, f, mine=False):
        for dy in range(1, ny):
            act(copy(c, f, 1 + dy, fs_at(z, dy), mine))

    def local(c):
        return pltpu.make_async_copy(own(c), piece(c, me), local_sem.at[c])

    barrier = pltpu.get_barrier_semaphore()
    greet = [lax.rem(me + ny, n_fs), lax.rem(me + n_fs - ny, n_fs)]
    greet += [fs_at(z, dy) for dy in range(1, ny)]
    for other in greet:
        pl.semaphore_signal(barrier, inc=1, device_id={"fs": other}, device_id_type=MESH)
    pl.semaphore_wait(barrier, len(greet))

    def walk(act, wait):
        for c in range(len(plan)):
            y_sends(act, c, me, True)
            z_sends(act, c, me, True, True, True)
        if wait:
            for c in range(len(plan)):
                local(c).start()
        for c in range(len(plan)):
            if plan[c][5]:
                for dy in range(1, ny):
                    f = fs_at(z, dy)
                    if wait:
                        arrived(c, f)
                    z_sends(act, c, f, True, True)
        for t in range(1, nz):
            for c in range(len(plan)):
                for below in (True, False):
                    zz = z - t if below else z + t

                    @pl.when(zz >= 0 if below else zz < nz)
                    def _():
                        for dy in range(ny) if plan[c][5] else (0,):
                            f = fs_at(zz, dy)
                            if wait:
                                arrived(c, f)
                            z_sends(act, c, f, below, not below)
                            if not plan[c][5]:
                                y_sends(act, c, f)

    walk(lambda d: d.start(), True)
    for c in range(len(plan)):
        if not plan[c][5]:
            for zz in range(nz):
                for dy in range(1, ny):
                    arrived(c, fs_at(zz, dy))
        local(c).wait()
    walk(lambda d: d.wait_send(), False)


def fs_gather(shards, axes, chunks, y_first, nz, ny, ident):
    n_fs = nz * ny
    plan, shapes = [], []
    for m, (w, axis) in enumerate(zip(shards, axes)):
        block = w.shape[axis]
        size = max(128, block // chunks)
        size = size if block % size == 0 else block
        for off in range(0, block, size):
            plan.append((m, axis, block, off, size, len(plan) < y_first and block > size))
        shape = list(w.shape)
        shape[axis] = block * n_fs
        shapes.append(jax.ShapeDtypeStruct(tuple(shape), w.dtype))
    n = len(plan)
    return pl.pallas_call(
        functools.partial(gather_kernel, nz, ny, tuple(plan), len(shards)),
        out_shape=shapes,
        in_specs=[pl.BlockSpec(memory_space=pl.ANY)] * len(shards),
        out_specs=[pl.BlockSpec(memory_space=pl.ANY)] * len(shards),
        scratch_shapes=[
            pltpu.SemaphoreType.DMA((1 + ny, n_fs, n)),
            pltpu.SemaphoreType.DMA((n_fs, n)),
            pltpu.SemaphoreType.DMA((n,)),
        ],
        compiler_params=pltpu.CompilerParams(collective_id=ident, has_side_effects=True),
        cost_estimate=pl.CostEstimate(flops=10**11, bytes_accessed=10**7, transcendentals=0),
    )(*shards)


def make_body(n_fs, n_tp, ny):
    nz, nx = n_fs // ny, n_tp // 2

    def hop_x(a, dx):
        return lax.ppermute(
            a, "tp", [(x * 2 + c, (x + dx) % nx * 2 + c) for x in range(nx) for c in range(2)]
        )

    def hop_core(a):
        return lax.ppermute(a, "tp", [(t, t ^ 1) for t in range(n_tp)])

    def body(
        mixed,
        residual,
        mix_weight,
        norm_gain,
        up_weight,
        gate_weight,
        conv_weight,
        conv_bias,
        down_weight,
    ):
        tp_i = lax.axis_index("tp")
        core, x_i = tp_i % 2, tp_i // 2
        tok, width = residual.shape
        mix_full = lax.all_gather(mix_weight, ("fs", "tp"), axis=0, tiled=True)
        up_full, gate_full = fs_gather((up_weight, gate_weight), (0, 0), 2, 1, nz, ny, 0)
        mix_full, up_full = lax.optimization_barrier((mix_full, up_full))
        summed = jnp.dot(mixed, mix_full, preferred_element_type=f32)
        stream = (residual.astype(f32) + summed).astype(bf16)
        x_float = stream.astype(f32)
        normed = (
            x_float
            * lax.rsqrt(jnp.mean(x_float * x_float, axis=-1, keepdims=True) + norm_eps)
            * norm_gain
        ).astype(bf16)
        normed, down_weight = lax.optimization_barrier((normed, down_weight))
        tokens = lax.all_gather(normed, "tp", axis=0, tiled=True)
        (down_full,) = fs_gather((down_weight,), (1,), 2, 0, nz, ny, 1)
        tokens, down_full = lax.optimization_barrier((tokens, down_full))
        up_part = jnp.dot(tokens, up_full, preferred_element_type=f32).astype(bf16)
        gate_part = jnp.dot(tokens, gate_full, preferred_element_type=f32).astype(bf16)
        up_float = lax.optimization_barrier(up_part).astype(f32)
        padded = jnp.pad(up_float, ((2, 0), (0, 0)))
        smoothed = (
            conv_bias
            + conv_weight[0] * padded[:-2]
            + conv_weight[1] * padded[1:-1]
            + conv_weight[2] * padded[2:]
        )
        hidden = (jax.nn.gelu(smoothed) * gate_part.astype(f32)).astype(bf16)
        hidden = lax.optimization_barrier(hidden)
        pieces = 2
        wide = width // pieces
        sums = []
        for c in range(pieces):
            part = jnp.dot(
                hidden, down_full[:, c * wide : (c + 1) * wide], preferred_element_type=f32
            ).astype(bf16)
            part = part.reshape(nx, 2, tok, wide)
            theirs = lax.dynamic_index_in_dim(part, 1 - core, 1, keepdims=False)
            ours = lax.dynamic_index_in_dim(part, core, 1, keepdims=False)
            pair = (ours.astype(f32) + hop_core(theirs).astype(f32)).astype(bf16)
            total = lax.dynamic_index_in_dim(pair, x_i, 0, keepdims=False).astype(f32)
            for dx in range(1, nx):
                away = lax.dynamic_index_in_dim(pair, (x_i + dx) % nx, 0, keepdims=False)
                total = total + hop_x(away, dx).astype(f32)
            sums.append(total)
        return (x_float + jnp.concatenate(sums, axis=1)).astype(bf16)

    return body


def solution(mesh):
    coords = [getattr(d, "coords", None) for d in mesh.devices[:, 0]]
    n_fs, n_tp = mesh.shape["fs"], mesh.shape["tp"]
    ny = len({c[1] for c in coords}) if None not in coords else 1
    if n_fs % ny:
        ny = 1
    return jax.shard_map(
        make_body(n_fs, n_tp, ny),
        mesh=mesh,
        in_specs=(
            P(("fs", "tp"), None),
            P(("fs", "tp"), None),
            P(("fs", "tp"), None),
            P(),
            P("fs", "tp"),
            P("fs", "tp"),
            P(None, "tp"),
            P("tp"),
            P("tp", "fs"),
        ),
        out_specs=P(("fs", "tp"), None),
        check_vma=False,
    )
```

```python
import functools

import jax
import jax.numpy as jnp
from jax import lax
from jax.experimental import pallas as pl
from jax.experimental.pallas import tpu as pltpu
from jax.sharding import PartitionSpec as P


norm_eps = 1e-06
f32, bf16 = jnp.float32, jnp.bfloat16
MESH = pl.DeviceIdType.MESH


def gather_kernel(nz, ny, nx, plan, count, spread, *refs):
    shards, fulls = refs[:count], refs[count : 2 * count]
    send_sem, recv_sem, local_sem, tp_send, tp_recv = refs[2 * count :]
    n_fs = nz * ny
    me = lax.axis_index("fs")
    z, y = me // ny, lax.rem(me, ny)
    tp = lax.axis_index("tp")
    x, core = tp // 2, lax.rem(tp, 2)

    def x_at(dx):
        return lax.rem(x + dx, nx) * 2 + core

    def fs_at(zz, dy):
        return zz * ny + lax.rem(y + dy, ny)

    def part(f, t):
        rows = plan[0][4]
        return fulls[0].at[pl.ds(pl.multiple_of((f * (2 * nx) + t) * rows, 16), rows), :]

    def piece(c, f):
        m, axis, block, off, size, _ = plan[c]
        if spread and c == 0:
            return part(f, tp)
        if axis == 0:
            return fulls[m].at[pl.ds(pl.multiple_of(f * block + off, 16), size), :]
        return fulls[m].at[:, pl.ds(pl.multiple_of(f * block + off, 128), size)]

    def own(c):
        m, axis, _, off, size, _ = plan[c]
        return shards[m].at[off : off + size, :] if axis == 0 else shards[m].at[:, off : off + size]

    def copy(c, f, lane, to, mine=False):
        return pltpu.make_async_remote_copy(
            src_ref=own(c) if mine else piece(c, f),
            dst_ref=piece(c, f),
            send_sem=send_sem.at[lane, f, c],
            recv_sem=recv_sem.at[f, c],
            device_id={"fs": to},
            device_id_type=MESH,
        )

    def arrived(c, f):
        copy(c, f, 0, lax.rem(me + 1, n_fs)).wait_recv()

    def z_sends(act, c, f, up, down, mine=False):
        if up:

            @pl.when(z < nz - 1)
            def _():
                act(copy(c, f, 0, me + ny, mine))

        if down:

            @pl.when(z > 0)
            def _():
                act(copy(c, f, 1, me - ny, mine))

    def y_sends(act, c, f, mine=False):
        for dy in range(1, ny):
            act(copy(c, f, 1 + dy, fs_at(z, dy), mine))

    def tp_copy(f, t, lane, to):
        return pltpu.make_async_remote_copy(
            src_ref=part(f, t),
            dst_ref=part(f, t),
            send_sem=tp_send.at[f, lane],
            recv_sem=tp_recv.at[f, t],
            device_id={"tp": to},
            device_id_type=MESH,
        )

    def tp_sends(act, f):
        for dx in range(1, nx):
            act(tp_copy(f, tp, dx - 1, x_at(dx)))
        act(tp_copy(f, tp, nx - 1, tp + 1 - 2 * core))

    def tp_relay(act, f, wait):
        for dx in range(1, nx):
            if wait:
                tp_copy(f, x_at(dx), 0, x_at(dx)).wait_recv()
            act(tp_copy(f, x_at(dx), nx - 1 + dx, tp + 1 - 2 * core))

    def local(c):
        return pltpu.make_async_copy(own(c), piece(c, me), local_sem.at[c])

    barrier = pltpu.get_barrier_semaphore()
    greet = [lax.rem(me + ny, n_fs), lax.rem(me + n_fs - ny, n_fs)]
    greet += [fs_at(z, dy) for dy in range(1, ny)]
    for other in greet:
        pl.semaphore_signal(barrier, inc=1, device_id={"fs": other}, device_id_type=MESH)
    greet_tp = [x_at(dx) for dx in range(1, nx)] + [tp + 1 - 2 * core] if spread else []
    for other in greet_tp:
        pl.semaphore_signal(barrier, inc=1, device_id={"tp": other}, device_id_type=MESH)
    pl.semaphore_wait(barrier, len(greet) + len(greet_tp))

    def walk(act, wait):
        for c in range(len(plan)):
            y_sends(act, c, me, True)
            z_sends(act, c, me, True, True, True)
        if wait:
            for c in range(len(plan)):
                local(c).start()
        if spread:
            if wait:
                local(0).wait()
            tp_sends(act, me)
        for c in range(len(plan)):
            if plan[c][5]:
                for dy in range(1, ny):
                    f = fs_at(z, dy)
                    if wait:
                        arrived(c, f)
                    z_sends(act, c, f, True, True)

        def from_y(zz):
            for dy in range(1, ny):
                f = fs_at(zz, dy)
                if wait:
                    arrived(0, f)
                tp_sends(act, f)

        def both(t, do):
            for below in (True, False) if t else (True,):
                zz = z - t if below else z + t
                pl.when(zz >= 0 if below else zz < nz)(functools.partial(do, zz))

        for t in range(1, nz):
            if spread:
                both(t - 1, from_y)
            for c in range(len(plan)):
                for below in (True, False):
                    zz = z - t if below else z + t

                    @pl.when(zz >= 0 if below else zz < nz)
                    def _():
                        for dy in range(ny) if plan[c][5] else (0,):
                            f = fs_at(zz, dy)
                            if wait:
                                arrived(c, f)
                            z_sends(act, c, f, below, not below)
                            if not plan[c][5]:
                                y_sends(act, c, f)
                            if spread and c == 0:
                                tp_sends(act, f)

        if spread:
            both(nz - 1, from_y)
            for f in range(n_fs):
                tp_relay(act, f, wait)

    walk(lambda d: d.start(), True)
    if spread:
        for f in range(n_fs):
            for dx in range(nx):
                t = x_at(dx) + 1 - 2 * core
                tp_copy(f, t, 0, tp + 1 - 2 * core).wait_recv()
    for c in range(1 if spread else 0, len(plan)):
        if not plan[c][5]:
            for zz in range(nz):
                for dy in range(1, ny):
                    arrived(c, fs_at(zz, dy))
    for c in range(1 if spread else 0, len(plan)):
        local(c).wait()
    walk(lambda d: d.wait_send(), False)


def fs_gather(shards, axes, chunks, y_first, nz, ny, nx, spread, ident):
    n_fs = nz * ny
    plan, shapes = [], []
    for m, (w, axis) in enumerate(zip(shards, axes)):
        block = w.shape[axis]
        size = max(128, block // chunks)
        size = size if block % size == 0 else block
        for off in range(0, block, size):
            plan.append((m, axis, block, off, size, len(plan) in y_first and block > size))
        shape = list(w.shape)
        shape[axis] = block * n_fs * (2 * nx if spread and m == 0 else 1)
        shapes.append(jax.ShapeDtypeStruct(tuple(shape), w.dtype))
    n = len(plan)
    return pl.pallas_call(
        functools.partial(gather_kernel, nz, ny, nx, tuple(plan), len(shards), spread),
        out_shape=shapes,
        in_specs=[pl.BlockSpec(memory_space=pl.ANY)] * len(shards),
        out_specs=[pl.BlockSpec(memory_space=pl.ANY)] * len(shards),
        scratch_shapes=[
            pltpu.SemaphoreType.DMA((1 + ny, n_fs, n)),
            pltpu.SemaphoreType.DMA((n_fs, n)),
            pltpu.SemaphoreType.DMA((n,)),
            pltpu.SemaphoreType.DMA((n_fs, 2 * nx - 1)),
            pltpu.SemaphoreType.DMA((n_fs, 2 * nx)),
        ],
        compiler_params=pltpu.CompilerParams(collective_id=ident, has_side_effects=True),
        cost_estimate=pl.CostEstimate(flops=10**11, bytes_accessed=10**7, transcendentals=0),
    )(*shards)


def make_body(n_fs, n_tp, ny):
    nz, nx = n_fs // ny, n_tp // 2

    def hop_x(a, dx):
        return lax.ppermute(
            a, "tp", [(x * 2 + c, (x + dx) % nx * 2 + c) for x in range(nx) for c in range(2)]
        )

    def hop_core(a):
        return lax.ppermute(a, "tp", [(t, t ^ 1) for t in range(n_tp)])

    def body(
        mixed,
        residual,
        mix_weight,
        norm_gain,
        up_weight,
        gate_weight,
        conv_weight,
        conv_bias,
        down_weight,
    ):
        tp_i = lax.axis_index("tp")
        core, x_i = tp_i % 2, tp_i // 2
        tok, width = residual.shape
        mix_full, up_full, gate_full = fs_gather(
            (mix_weight, up_weight, gate_weight), (0, 0, 0), 2, (1,), nz, ny, nx, True, 0
        )
        summed = jnp.dot(mixed, mix_full, preferred_element_type=f32)
        stream = (residual.astype(f32) + summed).astype(bf16)
        x_float = stream.astype(f32)
        normed = (
            x_float
            * lax.rsqrt(jnp.mean(x_float * x_float, axis=-1, keepdims=True) + norm_eps)
            * norm_gain
        ).astype(bf16)
        normed, down_weight = lax.optimization_barrier((normed, down_weight))
        tokens = lax.all_gather(normed, "tp", axis=0, tiled=True)
        (down_full,) = fs_gather((down_weight,), (1,), 2, (), nz, ny, nx, False, 1)
        tokens, down_full = lax.optimization_barrier((tokens, down_full))
        lead = 16
        tokens = jnp.pad(tokens, ((lead, 0), (0, 0)))
        total, gate_tie = x_float, up_full
        for dx in list(range(1, nx)) + [0]:
            first = (x_i + dx) % nx * 2 * tok
            rows = lax.dynamic_slice_in_dim(tokens, first, 2 * tok + lead, axis=0)
            up_part = jnp.dot(rows, gate_tie, preferred_element_type=f32).astype(bf16)
            gate_part = jnp.dot(rows[lead:], gate_full, preferred_element_type=f32).astype(bf16)
            up_part = lax.optimization_barrier(up_part)
            smoothed = conv_bias
            for k in range(3):
                back = lead - 2 + k
                smoothed = smoothed + conv_weight[k] * up_part[back : back + 2 * tok].astype(f32)
            hidden = (jax.nn.gelu(smoothed) * gate_part.astype(f32)).astype(bf16)
            part = jnp.dot(hidden, down_full, preferred_element_type=f32).astype(bf16)
            part = part.reshape(2, tok, width)
            theirs = lax.dynamic_index_in_dim(part, 1 - core, 0, keepdims=False)
            ours = lax.dynamic_index_in_dim(part, core, 0, keepdims=False)
            pair = ours.astype(f32) + hop_core(theirs).astype(f32)
            if dx:
                pair = pair.astype(bf16)
                pair, gate_tie = lax.optimization_barrier((pair, gate_tie))
                pair = hop_x(pair, dx)
                pair = pair.astype(f32)
            total = total + pair
        return total.astype(bf16)

    return body


def solution(mesh):
    coords = [getattr(d, "coords", None) for d in mesh.devices[:, 0]]
    n_fs, n_tp = mesh.shape["fs"], mesh.shape["tp"]
    ny = len({c[1] for c in coords}) if None not in coords else 1
    if n_fs % ny:
        ny = 1
    return jax.shard_map(
        make_body(n_fs, n_tp, ny),
        mesh=mesh,
        in_specs=(
            P(("fs", "tp"), None),
            P(("fs", "tp"), None),
            P(("fs", "tp"), None),
            P(),
            P("fs", "tp"),
            P("fs", "tp"),
            P(None, "tp"),
            P("tp"),
            P("tp", "fs"),
        ),
        out_specs=P(("fs", "tp"), None),
        check_vma=False,
    )
```

```python
import functools

import jax
import jax.numpy as jnp
from jax import lax
from jax.experimental import pallas as pl
from jax.experimental.pallas import tpu as pltpu
from jax.sharding import PartitionSpec as P


norm_eps = 1e-06
f32, bf16 = jnp.float32, jnp.bfloat16
MESH = pl.DeviceIdType.MESH


def gather_kernel(nz, ny, nx, plan, count, spread, share, *refs):
    shards, fulls = refs[:count], refs[count : 2 * count]
    send_sem, recv_sem, local_sem, tp_send, tp_recv = refs[2 * count :]
    n_fs = nz * ny
    me = lax.axis_index("fs")
    z, y = me // ny, lax.rem(me, ny)
    tp = lax.axis_index("tp")
    x, core = tp // 2, lax.rem(tp, 2)

    def x_at(dx):
        return lax.rem(x + dx, nx) * 2 + core

    def fs_at(zz, dy):
        return zz * ny + lax.rem(y + dy, ny)

    def part(f, t):
        rows = plan[0][4]
        return fulls[0].at[pl.ds(pl.multiple_of((f * (2 * nx) + t) * rows, 16), rows), :]

    def piece(c, f):
        m, axis, block, off, size, _ = plan[c]
        if spread and c == 0:
            return part(f, tp)
        if axis == 0:
            return fulls[m].at[pl.ds(pl.multiple_of(f * block + off, 16), size), :]
        return fulls[m].at[:, pl.ds(pl.multiple_of(f * block + off, 128), size)]

    def own(c):
        m, axis, _, off, size, _ = plan[c]
        return shards[m].at[off : off + size, :] if axis == 0 else shards[m].at[:, off : off + size]

    def copy(c, f, lane, to, mine=False):
        return pltpu.make_async_remote_copy(
            src_ref=own(c) if mine else piece(c, f),
            dst_ref=piece(c, f),
            send_sem=send_sem.at[lane, f, c],
            recv_sem=recv_sem.at[f, c],
            device_id={"fs": to},
            device_id_type=MESH,
        )

    def arrived(c, f):
        copy(c, f, 0, lax.rem(me + 1, n_fs)).wait_recv()

    def z_sends(act, c, f, up, down, mine=False):
        if up:

            @pl.when(z < nz - 1)
            def _():
                act(copy(c, f, 0, me + ny, mine))

        if down:

            @pl.when(z > 0)
            def _():
                act(copy(c, f, 1, me - ny, mine))

    def y_sends(act, c, f, mine=False):
        for dy in range(1, ny):
            act(copy(c, f, 1 + dy, fs_at(z, dy), mine))

    def tp_copy(f, t, lane, to):
        return pltpu.make_async_remote_copy(
            src_ref=part(f, t),
            dst_ref=part(f, t),
            send_sem=tp_send.at[f, lane],
            recv_sem=tp_recv.at[f, t],
            device_id={"tp": to},
            device_id_type=MESH,
        )

    def tp_sends(act, f):
        for dx in range(1, nx):
            act(tp_copy(f, tp, dx - 1, x_at(dx)))
        act(tp_copy(f, tp, nx - 1, tp + 1 - 2 * core))

    def tp_relay(act, f, wait):
        for dx in range(1, nx):
            if wait:
                tp_copy(f, x_at(dx), 0, x_at(dx)).wait_recv()
            act(tp_copy(f, x_at(dx), nx - 1 + dx, tp + 1 - 2 * core))

    def shared(t):
        rows = shards[-1].shape[0]
        return fulls[-1].at[pl.ds(pl.multiple_of(t * rows, 16), rows), :]

    def share_copy(t, lane, to, mine=False):
        return pltpu.make_async_remote_copy(
            src_ref=shards[-1] if mine else shared(t),
            dst_ref=shared(t),
            send_sem=tp_send.at[0, lane],
            recv_sem=tp_recv.at[0, t],
            device_id={"tp": to},
            device_id_type=MESH,
        )

    def share_local():
        return pltpu.make_async_copy(shards[-1], shared(tp), local_sem.at[len(plan)])

    def local(c):
        return pltpu.make_async_copy(own(c), piece(c, me), local_sem.at[c])

    barrier = pltpu.get_barrier_semaphore()
    greet = [lax.rem(me + ny, n_fs), lax.rem(me + n_fs - ny, n_fs)]
    greet += [fs_at(z, dy) for dy in range(1, ny)]
    for other in greet:
        pl.semaphore_signal(barrier, inc=1, device_id={"fs": other}, device_id_type=MESH)
    greet_tp = [x_at(dx) for dx in range(1, nx)] + [tp + 1 - 2 * core]
    greet_tp = greet_tp if spread or share else []
    for other in greet_tp:
        pl.semaphore_signal(barrier, inc=1, device_id={"tp": other}, device_id_type=MESH)
    pl.semaphore_wait(barrier, len(greet) + len(greet_tp))

    def walk(act, wait):
        if share:
            for dx in range(1, nx):
                act(share_copy(tp, dx - 1, x_at(dx), True))
            act(share_copy(tp, nx - 1, tp + 1 - 2 * core, True))
            if wait:
                share_local().start()
        for c in range(len(plan)):
            y_sends(act, c, me, True)
            z_sends(act, c, me, True, True, True)
        if wait:
            for c in range(len(plan)):
                local(c).start()
        if spread:
            if wait:
                local(0).wait()
            tp_sends(act, me)
        for c in range(len(plan)):
            if plan[c][5]:
                for dy in range(1, ny):
                    f = fs_at(z, dy)
                    if wait:
                        arrived(c, f)
                    z_sends(act, c, f, True, True)

        def from_y(zz):
            for dy in range(1, ny):
                f = fs_at(zz, dy)
                if wait:
                    arrived(0, f)
                tp_sends(act, f)

        def both(t, do):
            for below in (True, False) if t else (True,):
                zz = z - t if below else z + t
                pl.when(zz >= 0 if below else zz < nz)(functools.partial(do, zz))

        for t in range(1, nz):
            if spread:
                both(t - 1, from_y)
            for c in range(len(plan)):
                for below in (True, False):
                    zz = z - t if below else z + t

                    @pl.when(zz >= 0 if below else zz < nz)
                    def _():
                        for dy in range(ny) if plan[c][5] else (0,):
                            f = fs_at(zz, dy)
                            if wait:
                                arrived(c, f)
                            z_sends(act, c, f, below, not below)
                            if not plan[c][5]:
                                y_sends(act, c, f)
                            if spread and c == 0:
                                tp_sends(act, f)

        if share:
            for dx in range(1, nx):
                if wait:
                    share_copy(x_at(dx), 0, x_at(dx)).wait_recv()
                act(share_copy(x_at(dx), nx - 1 + dx, tp + 1 - 2 * core))
        if spread:
            both(nz - 1, from_y)
            for f in range(n_fs):
                tp_relay(act, f, wait)

    walk(lambda d: d.start(), True)
    if share:
        for dx in range(nx):
            t = x_at(dx) + 1 - 2 * core
            share_copy(t, 0, tp + 1 - 2 * core).wait_recv()
        share_local().wait()
    if spread:
        for f in range(n_fs):
            for dx in range(nx):
                t = x_at(dx) + 1 - 2 * core
                tp_copy(f, t, 0, tp + 1 - 2 * core).wait_recv()
    for c in range(1 if spread else 0, len(plan)):
        if not plan[c][5]:
            for zz in range(nz):
                for dy in range(1, ny):
                    arrived(c, fs_at(zz, dy))
    for c in range(1 if spread else 0, len(plan)):
        local(c).wait()
    walk(lambda d: d.wait_send(), False)


def fs_gather(shards, axes, chunks, y_first, nz, ny, nx, spread, ident, rows=None):
    n_fs = nz * ny
    plan, shapes = [], []
    for m, (w, axis) in enumerate(zip(shards, axes)):
        block = w.shape[axis]
        size = max(128, block // chunks)
        size = size if block % size == 0 else block
        for off in range(0, block, size):
            plan.append((m, axis, block, off, size, len(plan) in y_first and block > size))
        shape = list(w.shape)
        shape[axis] = block * n_fs * (2 * nx if spread and m == 0 else 1)
        shapes.append(jax.ShapeDtypeStruct(tuple(shape), w.dtype))
    if rows is not None:
        shards = (*shards, rows)
        shapes.append(jax.ShapeDtypeStruct((rows.shape[0] * 2 * nx, rows.shape[1]), rows.dtype))
    n = len(plan)
    return pl.pallas_call(
        functools.partial(gather_kernel, nz, ny, nx, tuple(plan), len(shards), spread, rows is not None),
        out_shape=shapes,
        in_specs=[pl.BlockSpec(memory_space=pl.ANY)] * len(shards),
        out_specs=[pl.BlockSpec(memory_space=pl.ANY)] * len(shards),
        scratch_shapes=[
            pltpu.SemaphoreType.DMA((1 + ny, n_fs, n)),
            pltpu.SemaphoreType.DMA((n_fs, n)),
            pltpu.SemaphoreType.DMA((n + 1,)),
            pltpu.SemaphoreType.DMA((n_fs, 2 * nx - 1)),
            pltpu.SemaphoreType.DMA((n_fs, 2 * nx)),
        ],
        compiler_params=pltpu.CompilerParams(collective_id=ident, has_side_effects=True),
        cost_estimate=pl.CostEstimate(flops=10**11, bytes_accessed=10**7, transcendentals=0),
    )(*shards)


def make_body(n_fs, n_tp, ny):
    nz, nx = n_fs // ny, n_tp // 2

    def hop_x(a, dx):
        return lax.ppermute(
            a, "tp", [(x * 2 + c, (x + dx) % nx * 2 + c) for x in range(nx) for c in range(2)]
        )

    def hop_core(a):
        return lax.ppermute(a, "tp", [(t, t ^ 1) for t in range(n_tp)])

    def body(
        mixed,
        residual,
        mix_weight,
        norm_gain,
        up_weight,
        gate_weight,
        conv_weight,
        conv_bias,
        down_weight,
    ):
        tp_i = lax.axis_index("tp")
        core, x_i = tp_i % 2, tp_i // 2
        tok, width = residual.shape
        mix_full, up_full, gate_full = fs_gather(
            (mix_weight, up_weight, gate_weight), (0, 0, 0), 2, (1,), nz, ny, nx, True, 0
        )
        summed = jnp.dot(mixed, mix_full, preferred_element_type=f32)
        stream = (residual.astype(f32) + summed).astype(bf16)
        x_float = stream.astype(f32)
        normed = (
            x_float
            * lax.rsqrt(jnp.mean(x_float * x_float, axis=-1, keepdims=True) + norm_eps)
            * norm_gain
        ).astype(bf16)
        down_full, tokens = fs_gather(
            (down_weight,), (1,), 2, (), nz, ny, nx, False, 1, normed
        )
        lead = 16
        tokens = jnp.pad(tokens, ((lead, 0), (0, 0)))
        total, gate_tie = x_float, up_full
        for dx in list(range(1, nx)) + [0]:
            first = (x_i + dx) % nx * 2 * tok
            rows = lax.dynamic_slice_in_dim(tokens, first, 2 * tok + lead, axis=0)
            up_part = jnp.dot(rows, gate_tie, preferred_element_type=f32).astype(bf16)
            gate_part = jnp.dot(rows[lead:], gate_full, preferred_element_type=f32).astype(bf16)
            up_part = lax.optimization_barrier(up_part)
            smoothed = conv_bias
            for k in range(3):
                back = lead - 2 + k
                smoothed = smoothed + conv_weight[k] * up_part[back : back + 2 * tok].astype(f32)
            hidden = (jax.nn.gelu(smoothed) * gate_part.astype(f32)).astype(bf16)
            part = jnp.dot(hidden, down_full, preferred_element_type=f32).astype(bf16)
            part = part.reshape(2, tok, width)
            theirs = lax.dynamic_index_in_dim(part, 1 - core, 0, keepdims=False)
            ours = lax.dynamic_index_in_dim(part, core, 0, keepdims=False)
            pair = ours.astype(f32) + hop_core(theirs).astype(f32)
            if dx:
                pair = pair.astype(bf16)
                pair, gate_tie = lax.optimization_barrier((pair, gate_tie))
                pair = hop_x(pair, dx)
                pair = pair.astype(f32)
            total = total + pair
        return total.astype(bf16)

    return body


def solution(mesh):
    coords = [getattr(d, "coords", None) for d in mesh.devices[:, 0]]
    n_fs, n_tp = mesh.shape["fs"], mesh.shape["tp"]
    ny = len({c[1] for c in coords}) if None not in coords else 1
    if n_fs % ny:
        ny = 1
    return jax.shard_map(
        make_body(n_fs, n_tp, ny),
        mesh=mesh,
        in_specs=(
            P(("fs", "tp"), None),
            P(("fs", "tp"), None),
            P(("fs", "tp"), None),
            P(),
            P("fs", "tp"),
            P("fs", "tp"),
            P(None, "tp"),
            P("tp"),
            P("tp", "fs"),
        ),
        out_specs=P(("fs", "tp"), None),
        check_vma=False,
    )
```
